32 devices in a mesh: sp: 4 (over z), dp: 8 (over y, x, core).
Axes of the slice: x: 2, y: 2, z: 4, core: 2. Of those that a mesh axis runs over, the one named last changes fastest.
Arguments:
- queries: bfloat16 [8, 512, 1024], P('dp', 'sp'), may hold values from -6 to 6
- key_rows: bfloat16 [8, 512, 1024], P('dp', 'sp'), may hold values from -6 to 6
- values: bfloat16 [8, 512, 2048], P('dp', 'sp'), may hold values from -6 to 6
- out_gate: bfloat16 [8, 512, 2048], P('dp', 'sp'), may hold values from -6 to 6
- input_gate: bfloat16 [8, 4, 512], P('dp', None, 'sp'), may hold values from -6 to 205
- forget_gate: bfloat16 [8, 4, 512], P('dp', None, 'sp'), may hold values from 0.5 to 13
- out_weight: bfloat16 [2048, 2048], P(None, 'dp'), may hold values from -0.125 to 0.125
Outputs:
- layer_out: bfloat16 [8, 512, 2048], P('dp', 'sp')
The draws below stay inside these ranges and needn't reach their ends.
All inputs are finite; a program needn't handle non-finite values.
Results may differ from the reference program's by a relative error of at most 0.0057.
Values may be sent and summed in bfloat16 or wider, within the bound.
A program may use at most 64 MiB of HBM per device.

```python
import jax
import jax.numpy as jnp
from jax import lax

D = 2048
MEMORY_UNITS = 4
DK = 256
DV = 512
BLOCK = 128
TOK_DEV = 128
STEP_TOTAL = 512
STREAM_TOTAL = 8
VW = 2048


def draw_input_gate(key, part):
    dims_all = (STREAM_TOTAL, MEMORY_UNITS, STEP_TOTAL)
    result = jnp.clip(1.5 * jax.random.normal(jax.random.fold_in(key, 4), dims_all, jnp.float32), -6.0, 6.0)
    return result.astype(jnp.bfloat16)


def draw_forget_gate(key, part):
    dims_all = (STREAM_TOTAL, MEMORY_UNITS, STEP_TOTAL)
    multiplier = jnp.exp(jax.random.uniform(jax.random.fold_in(key, 11), (STREAM_TOTAL, MEMORY_UNITS, STEP_TOTAL // TOK_DEV, 1), jnp.float32, -0.7, 0.7))
    multiplier = jnp.broadcast_to(multiplier, (STREAM_TOTAL, MEMORY_UNITS, STEP_TOTAL // TOK_DEV, TOK_DEV)).reshape(dims_all)
    gaussian_jitter = jnp.exp(0.5 * jnp.clip(jax.random.normal(jax.random.fold_in(key, 12), dims_all, jnp.float32), -3.0, 3.0))
    ranking = jax.random.randint(jax.random.fold_in(key, 13), (STREAM_TOTAL, MEMORY_UNITS), 0, 1 << 20) * MEMORY_UNITS + lax.broadcasted_iota(jnp.int32, (STREAM_TOTAL, MEMORY_UNITS), 1)
    order = jnp.argsort(ranking, axis=1)
    position_rank = jnp.argsort(order, axis=1)
    quick_head = (position_rank < MEMORY_UNITS // 2)[:, :, None]
    background_level = jnp.where(quick_head, 1.0 / 40.0, 0.5 / STEP_TOTAL) * jnp.ones(dims_all, jnp.float32)
    spike_offset = jax.random.randint(jax.random.fold_in(key, 14), (STREAM_TOTAL, MEMORY_UNITS, 3, 1), 0, STEP_TOTAL)
    spike_indices = lax.broadcasted_iota(jnp.int32, (1, 1, 1, STEP_TOTAL), 3)
    spike_count = jnp.any(spike_indices == spike_offset, axis=2)
    spike_magnitude = jnp.where(spike_count, 0.4, background_level * multiplier * gaussian_jitter)
    gate_logits = -jnp.log(jnp.expm1(spike_magnitude))
    return gate_logits.astype(jnp.bfloat16)


def levels(rng, shape, cuts, smallest, high):
    def one(position, shards_of):
        steps = jax.random.uniform(jax.random.fold_in(jax.random.fold_in(rng, 6), position), (shards_of,), jnp.float32, smallest / len(cuts), high / len(cuts))
        return jnp.repeat(jnp.exp(steps), shape[position] // shards_of).reshape((-1,) + (1,) * (len(shape) - position - 1))

    gain = one(*cuts[0])
    for cut in cuts[1:]:
        gain = gain * one(*cut)
    return gain


def bell_draw(own_key, dims, width, bound, shards=(), dtype=jnp.bfloat16):
    entries = jax.random.normal(own_key, dims, jnp.float32) * width
    if len(shards) > 0:
        entries = levels(own_key, dims, shards, -0.22, 0.18) * entries
    return jnp.clip(entries, min=-bound, max=bound).astype(dtype)


def setup_inputs(seed: int = 0) -> dict:
    key_of = jax.random.split(jax.random.key(seed), 8)
    return {
        "queries": bell_draw(key_of[0], (STREAM_TOTAL, STEP_TOTAL, MEMORY_UNITS * DK), 1.0, 6.0, ((0, 8), (1, 4))),
        "key_rows": bell_draw(key_of[1], (STREAM_TOTAL, STEP_TOTAL, MEMORY_UNITS * DK), 1.0, 6.0, ((0, 8), (1, 4))),
        "values": bell_draw(key_of[2], (STREAM_TOTAL, STEP_TOTAL, VW), 1.0, 6.0, ((0, 8), (1, 4))),
        "out_gate": bell_draw(key_of[3], (STREAM_TOTAL, STEP_TOTAL, VW), 1.0, 6.0, ((0, 8), (1, 4))),
        "input_gate": draw_input_gate(jax.random.fold_in(key_of[7], 71), 0),
        "forget_gate": draw_forget_gate(jax.random.fold_in(key_of[7], 71), 0),
        "out_weight": bell_draw(key_of[6], (VW, D), VW ** -0.5, 0.125, ((1, 8),)),
    }


def memory_cell(query_rows, key_in, value_rows, input_log, forget_log):
    block_count = query_rows.shape[0] // BLOCK
    key_width = query_rows.shape[1]
    value_width = value_rows.shape[1]
    key_scale = key_width ** -0.5
    causal = lax.broadcasted_iota(jnp.int32, (BLOCK, BLOCK), 0) >= lax.broadcasted_iota(jnp.int32, (BLOCK, BLOCK), 1)
    highest = lax.Precision.HIGHEST

    def block_step(state_in, inputs):
        memory, normer, stabil = state_in
        query_part, key_part, value_part, gain_part, decay_part = inputs
        query_part = query_part.astype(jnp.float32)
        key_part = key_part.astype(jnp.float32) * key_scale
        value_part = value_part.astype(jnp.float32)
        running = jnp.cumsum(decay_part)
        log_weight = running[:, None] - running[None, :] + gain_part[None, :]
        log_weight = jnp.where(causal, log_weight, -jnp.inf)
        carried_log = running + stabil
        row_top = jnp.maximum(carried_log, jnp.max(log_weight, axis=1))
        scores = jnp.dot(query_part, key_part.T, precision=highest) * jnp.exp(log_weight - row_top[:, None])
        carried = jnp.exp(carried_log - row_top)
        numerator = jnp.dot(scores, value_part, precision=highest) + carried[:, None] * jnp.dot(query_part, memory, precision=highest)
        denominator = jnp.sum(scores, axis=1) + carried * jnp.dot(query_part, normer, precision=highest)
        output = numerator / jnp.maximum(jnp.abs(denominator), 1.0)[:, None]
        block_end = running[-1]
        weight_log = block_end - running + gain_part
        new_top = jnp.maximum(block_end + stabil, jnp.max(weight_log))
        weights = jnp.exp(weight_log - new_top)
        retain = jnp.exp(block_end + stabil - new_top)
        memory = retain * memory + jnp.dot((key_part * weights[:, None]).T, value_part, precision=highest)
        normer = retain * normer + jnp.dot(weights, key_part, precision=highest)
        return (memory, normer, new_top), output

    start_state = (jnp.zeros((key_width, value_width), jnp.float32), jnp.zeros((key_width,), jnp.float32), jnp.zeros((), jnp.float32))
    blocks = tuple(source.reshape((block_count, BLOCK) + source.shape[1:]) for source in (query_rows, key_in, value_rows, input_log, forget_log))
    _, outputs = lax.scan(block_step, start_state, blocks)
    return outputs.reshape(block_count * BLOCK, value_width)


def reference(queries, key_rows, values, out_gate, input_gate, forget_gate, out_weight):
    query_heads = queries.reshape(STREAM_TOTAL, STEP_TOTAL, MEMORY_UNITS, DK).transpose(0, 2, 1, 3)
    key_heads = key_rows.reshape(STREAM_TOTAL, STEP_TOTAL, MEMORY_UNITS, DK).transpose(0, 2, 1, 3)
    value_heads = values.reshape(STREAM_TOTAL, STEP_TOTAL, MEMORY_UNITS, DV).transpose(0, 2, 1, 3)
    input_log = input_gate.astype(jnp.float32)
    forget_log = jax.nn.log_sigmoid(forget_gate.astype(jnp.float32))
    per_head = jax.vmap(jax.vmap(memory_cell))
    cell_out = per_head(query_heads, key_heads, value_heads, input_log, forget_log)
    hidden = cell_out.transpose(0, 2, 1, 3).reshape(STREAM_TOTAL, STEP_TOTAL, VW).astype(jnp.bfloat16)
    hidden = lax.optimization_barrier(hidden)
    gated = (hidden.astype(jnp.float32) * jax.nn.sigmoid(out_gate.astype(jnp.float32))).astype(jnp.bfloat16)
    projected = jnp.dot(gated.reshape(STREAM_TOTAL * STEP_TOTAL, VW), out_weight, preferred_element_type=jnp.float32)
    return projected.reshape(STREAM_TOTAL, STEP_TOTAL, D).astype(jnp.bfloat16)
```

```python
import functools

import jax
import jax.numpy as jnp
from jax import lax
from jax.experimental import pallas as pl
from jax.experimental.pallas import tpu as pltpu
from jax.sharding import PartitionSpec as P

F32 = jnp.float32
BF16 = jnp.bfloat16
MESH = pl.DeviceIdType.MESH
PIECES = 8
HIGHEST = lax.Precision.HIGHEST


def flip(index, bit):
    return index + bit * (1 - 2 * ((index // bit) % 2))


def split_dot(left, right):
    if right.dtype == BF16:
        return jnp.dot(left, right, preferred_element_type=F32)
    high = right.astype(BF16)
    low = (right - high.astype(F32)).astype(BF16)
    return jnp.dot(left, high, preferred_element_type=F32) + jnp.dot(
        left, low, preferred_element_type=F32
    )


def kernel(
    n_sp, n_dp, heads, gather,
    q_ref, k_ref, v_ref, gate_ref, in_ref, forget_ref, w_ref, o_ref,
    rows_ref, cols_ref, kw_ref, nloc_ref, kv_ref, num_ref, gated_ref,
    aux_in, aux_out, state_in, state_out, aux_sem, state_send, state_recv,
    *w_scratch,
):
    z = lax.axis_index("sp")
    d = lax.axis_index("dp")
    tokens = q_ref.shape[1]
    dk = q_ref.shape[2] // heads
    dv = v_ref.shape[2] // heads
    scale = dk ** (-0.5)
    total = state_in.shape[0]
    per_head = total // heads
    wide = state_in.shape[2]
    last = n_sp - 1

    barrier = pltpu.get_barrier_semaphore()
    count = 0
    if gather:
        for bit in (1, 2, 4):
            pl.semaphore_signal(barrier, 1, device_id={"dp": flip(d, bit)}, device_id_type=MESH)
        count = 3

    @pl.when(z > 0)
    def _():
        pl.semaphore_signal(barrier, 1, device_id={"sp": z - 1}, device_id_type=MESH)

    @pl.when(z < last)
    def _():
        pl.semaphore_signal(barrier, 1, device_id={"sp": z + 1}, device_id_type=MESH)

    count = count + jnp.where(z > 0, 1, 0) + jnp.where(z < last, 1, 0)
    pl.semaphore_wait(barrier, count)

    if gather:
        w_all, own_sem, w_send, w_recv = w_scratch
        core, xp, yp = flip(d, 1), flip(d, 2), flip(d, 4)
        diag = flip(xp, 4)
        core_x, core_y, core_diag = flip(xp, 1), flip(yp, 1), flip(diag, 1)
        deep = w_ref.shape[0] // PIECES
        half = PIECES // 2
        x_order = list(range(PIECES))
        y_order = x_order[half:] + x_order[:half]

        def part(piece):
            return pl.ds(piece * deep, deep)

        def copy_of(lane, piece, block, target, source=None):
            rows = part(piece)
            src = w_all.at[block, rows] if source is None else source.at[rows]
            return pltpu.make_async_remote_copy(
                src_ref=src,
                dst_ref=w_all.at[block, rows],
                send_sem=w_send.at[lane, piece],
                recv_sem=w_recv.at[lane, piece],
                device_id={"dp": target},
                device_id_type=MESH,
            )

        for x_piece, y_piece in zip(x_order, y_order):
            copy_of(0, x_piece, d, xp, w_ref).start()
            copy_of(1, y_piece, d, yp, w_ref).start()
        for piece in range(PIECES):
            copy_of(3, piece, d, core, w_ref).start()
        own = pltpu.make_async_copy(w_ref, w_all.at[d], own_sem)
        own.start()

        def pass_on(step):
            piece = x_order[step]
            copy_of(0, piece, xp, xp).wait_recv()
            copy_of(4, piece, xp, core).start()
            if step < half:
                copy_of(2, piece, xp, yp).start()
            piece = y_order[step]
            copy_of(1, piece, yp, yp).wait_recv()
            copy_of(5, piece, yp, core).start()
            if step < half:
                copy_of(2, piece, yp, xp).start()

    forget = forget_ref[0].astype(F32)
    gain = in_ref[0].astype(F32)
    decay = -(jnp.log1p(jnp.exp(-jnp.abs(forget))) + jnp.maximum(-forget, 0.0))
    row_id = lax.broadcasted_iota(jnp.int32, (tokens, tokens), 0)
    col_id = lax.broadcasted_iota(jnp.int32, (tokens, tokens), 1)
    running = jnp.dot(
        decay, (row_id <= col_id).astype(F32), precision=HIGHEST, preferred_element_type=F32
    )
    offset = gain - running
    end = running[:, tokens - 1 : tokens]
    top_here = end + jnp.max(offset, axis=1, keepdims=True)
    weight = jnp.exp(end + offset - top_here)
    rows_ref[...] = jnp.zeros_like(rows_ref)
    rows_ref[0:heads] = running
    rows_ref[heads : 2 * heads] = weight * scale
    cols_ref[...] = rows_ref[...].T

    for h in range(heads):
        keys = k_ref[0, :, h * dk : (h + 1) * dk].astype(F32)
        weighted = keys * cols_ref[:, heads + h : heads + h + 1]
        kw_ref[:, h * dk : (h + 1) * dk] = weighted.astype(BF16)
        nloc_ref[h : h + 1] = jnp.sum(weighted, axis=0, keepdims=True)

    def own_state(h):
        kv_ref[h] = lax.dot_general(
            kw_ref[:, h * dk : (h + 1) * dk],
            v_ref[0, :, h * dv : (h + 1) * dv],
            (((0,), (0,)), ((), ())),
            preferred_element_type=F32,
        )

    def aux_copy():
        return pltpu.make_async_remote_copy(
            src_ref=aux_out, dst_ref=aux_in, send_sem=aux_sem.at[0], recv_sem=aux_sem.at[1],
            device_id={"sp": jnp.minimum(z + 1, last)}, device_id_type=MESH,
        )

    def state_copy(j):
        return pltpu.make_async_remote_copy(
            src_ref=state_out.at[j], dst_ref=state_in.at[j],
            send_sem=state_send.at[j], recv_sem=state_recv.at[j],
            device_id={"sp": jnp.minimum(z + 1, last)}, device_id_type=MESH,
        )

    def aux_step(m, normer):
        top = jnp.maximum(end + m, top_here)
        keep = jnp.exp(end + m - top)
        add = jnp.exp(top_here - top)
        aux_out[0:heads] = keep * normer + add * nloc_ref[...]
        aux_out[heads : 2 * heads] = jnp.broadcast_to(top, (heads, dk))
        return keep, add

    def chunk_of(j):
        h, c = j // per_head, j % per_head
        return h, slice(c * wide, (c + 1) * wide), slice(h * dv + c * wide, h * dv + (c + 1) * wide)

    @pl.when(z == 0)
    def _():
        zero = jnp.zeros((heads, 1), F32)
        _, add = aux_step(zero, jnp.zeros((heads, dk), F32))
        aux_copy().start()
        for h in range(heads):
            own_state(h)
            for c in range(per_head):
                j = h * per_head + c
                _, inner, _ = chunk_of(j)
                state_out[j] = (add[h : h + 1] * kv_ref[h, :, inner]).astype(state_out.dtype)
                state_copy(j).start()
        aux_in[...] = jnp.zeros_like(aux_in)
        state_in[...] = jnp.zeros_like(state_in)

    @pl.when((z > 0) & (z < last))
    def _():
        for h in range(heads):
            own_state(h)

    tops, dens = [], []
    for h in range(heads):
        query = q_ref[0, :, h * dk : (h + 1) * dk]
        raw = lax.dot_general(
            query, k_ref[0, :, h * dk : (h + 1) * dk], (((1,), (1,)), ((), ())),
            preferred_element_type=F32,
        )
        log_weight = cols_ref[:, h : h + 1] + offset[h : h + 1]
        log_weight = jnp.where(row_id >= col_id, log_weight, -jnp.inf)
        top = jnp.max(log_weight, axis=1, keepdims=True)
        scores = (raw * scale) * jnp.exp(log_weight - top)
        tops.append(top)
        dens.append(jnp.sum(scores, axis=1, keepdims=True))
        high = scores.astype(BF16)
        low = (scores - high.astype(F32)).astype(BF16)
        value = v_ref[0, :, h * dv : (h + 1) * dv]
        num_ref[:, h * dv : (h + 1) * dv] = jnp.dot(
            high, value, preferred_element_type=F32
        ) + jnp.dot(low, value, preferred_element_type=F32)

    @pl.when(z > 0)
    def _():
        aux_copy().wait_recv()

    m = aux_in[heads : 2 * heads, 0:1]

    @pl.when((z > 0) & (z < last))
    def _():
        aux_step(m, aux_in[0:heads])
        aux_copy().start()

    top_next = jnp.maximum(end + m, top_here)
    keep = jnp.exp(end + m - top_next)
    add = jnp.exp(top_here - top_next)

    for j in range(total):
        h, inner, outer = chunk_of(j)
        if gather:
            for step in range(PIECES):
                place = [min(max(2 * step + 2 - 3 * s, 0), total - 1) for s in range(n_sp)]
                hits = [s for s in range(n_sp) if place[s] == j]
                if hits:

                    @pl.when((z >= hits[0]) & (z <= hits[-1]))
                    def _(step=step):
                        pass_on(step)

        @pl.when(z > 0)
        def _():
            state_copy(j).wait_recv()

        @pl.when((z > 0) & (z < last))
        def _():
            state_out[j] = (
                keep[h : h + 1] * state_in[j].astype(F32) + add[h : h + 1] * kv_ref[h, :, inner]
            ).astype(state_out.dtype)
            state_copy(j).start()

        query = q_ref[0, :, h * dk : (h + 1) * dk]
        if j % per_head == 0:
            carried = cols_ref[:, h : h + 1] + m[h : h + 1]
            top = jnp.maximum(carried, tops[h])
            local = jnp.exp(tops[h] - top)
            past = jnp.exp(carried - top)
            den = local * dens[h] + past * jnp.sum(
                query.astype(F32) * aux_in[h : h + 1], axis=1, keepdims=True
            )
            inverse = 1.0 / jnp.maximum(jnp.abs(den), 1.0)
            local, past = local * inverse, past * inverse
        cell = local * num_ref[:, outer] + past * split_dot(query, state_in[j])
        hidden = cell.astype(BF16).astype(F32)
        gate = jax.nn.sigmoid(gate_ref[0, :, outer].astype(F32))
        gated_ref[:, outer] = (hidden * gate).astype(BF16)

    if not gather:
        o_ref[0] = jnp.dot(gated_ref[...], w_ref[...], preferred_element_type=F32).astype(BF16)
    else:
        cols = w_ref.shape[1]

        def column(block):
            return pl.ds(pl.multiple_of(block * cols, cols), cols)

        def project(block):
            o_ref[0, :, column(block)] = jnp.dot(
                gated_ref[...], w_all[block], preferred_element_type=F32
            ).astype(BF16)

        own.wait()
        project(d)
        for piece in range(PIECES):
            copy_of(3, piece, core, core).wait_recv()
        project(core)
        project(xp)
        project(yp)
        for piece in range(PIECES):
            copy_of(4, piece, core_x, core).wait_recv()
        project(core_x)
        for piece in range(PIECES):
            copy_of(5, piece, core_y, core).wait_recv()
        project(core_y)
        mine = jnp.zeros((tokens, cols), F32)
        other = jnp.zeros((tokens, cols), F32)
        order = [p for pair in zip(x_order[:half], y_order[:half]) for p in pair]
        for piece in order:
            copy_of(2, piece, diag, yp).wait_recv()
            copy_of(6, piece, diag, core).start()
            rows = slice(piece * deep, (piece + 1) * deep)
            mine += jnp.dot(gated_ref[:, rows], w_all[diag, rows], preferred_element_type=F32)
        o_ref[0, :, column(diag)] = mine.astype(BF16)
        for piece in order:
            copy_of(6, piece, core_diag, core).wait_recv()
            rows = slice(piece * deep, (piece + 1) * deep)
            other += jnp.dot(gated_ref[:, rows], w_all[core_diag, rows], preferred_element_type=F32)
        o_ref[0, :, column(core_diag)] = other.astype(BF16)
        for piece in range(PIECES):
            copy_of(0, piece, d, xp, w_ref).wait_send()
            copy_of(1, piece, d, yp, w_ref).wait_send()
            copy_of(3, piece, d, core, w_ref).wait_send()
            copy_of(4, piece, xp, core).wait_send()
            copy_of(5, piece, yp, core).wait_send()
            copy_of(6, piece, diag, core).wait_send()
            copy_of(2, piece, xp if piece < half else yp, core).wait_send()

    @pl.when(z < last)
    def _():
        aux_copy().wait_send()
        for j in range(total):
            state_copy(j).wait_send()


def body(n_sp, n_dp, queries, key_rows, values, out_gate, input_gate, forget_gate, out_weight):
    heads = input_gate.shape[1]
    tokens = queries.shape[1]
    dk = queries.shape[2] // heads
    width = values.shape[2]
    dv = width // heads
    wide = min(128, dv)
    total = heads * (dv // wide)
    state_type = BF16 if n_sp <= 4 else F32
    depth, cols = out_weight.shape
    gather = n_dp == 8 and cols % 128 == 0
    scratch = [
        pltpu.VMEM((tokens, tokens), F32),
        pltpu.VMEM((tokens, tokens), F32),
        pltpu.VMEM((tokens, heads * dk), BF16),
        pltpu.VMEM((heads, dk), F32),
        pltpu.VMEM((heads, dk, dv), F32),
        pltpu.VMEM((tokens, width), F32),
        pltpu.VMEM((tokens, width), BF16),
        pltpu.VMEM((2 * heads, dk), F32),
        pltpu.VMEM((2 * heads, dk), F32),
        pltpu.VMEM((total, dk, wide), state_type),
        pltpu.VMEM((total, dk, wide), state_type),
        pltpu.SemaphoreType.DMA((2,)),
        pltpu.SemaphoreType.DMA((total,)),
        pltpu.SemaphoreType.DMA((total,)),
    ]
    vmem = pl.BlockSpec(memory_space=pltpu.VMEM)
    w_spec = vmem
    if gather:
        scratch += [
            pltpu.VMEM((n_dp, depth, cols), BF16),
            pltpu.SemaphoreType.DMA,
            pltpu.SemaphoreType.DMA((7, PIECES)),
            pltpu.SemaphoreType.DMA((7, PIECES)),
        ]
        w_spec = pl.BlockSpec(memory_space=pl.ANY)
    else:
        out_weight = lax.all_gather(out_weight, "dp", axis=1, tiled=True)
    out_width = cols * n_dp
    return pl.pallas_call(
        functools.partial(kernel, n_sp, n_dp, heads, gather),
        out_shape=jax.ShapeDtypeStruct((1, tokens, out_width), BF16),
        in_specs=[vmem] * 6 + [w_spec],
        out_specs=vmem,
        scratch_shapes=scratch,
        compiler_params=pltpu.CompilerParams(
            collective_id=0, has_side_effects=True, vmem_limit_bytes=56 * 1024 * 1024
        ),
    )(queries, key_rows, values, out_gate, input_gate, forget_gate, out_weight)


def solution(mesh):
    n_sp, n_dp = mesh.shape["sp"], mesh.shape["dp"]
    return jax.shard_map(
        functools.partial(body, n_sp, n_dp),
        mesh=mesh,
        in_specs=(
            P("dp", "sp", None),
            P("dp", "sp", None),
            P("dp", "sp", None),
            P("dp", "sp", None),
            P("dp", None, "sp"),
            P("dp", None, "sp"),
            P(None, "dp"),
        ),
        out_specs=P("dp", "sp", None),
        check_vma=False,
    )
```

```python
import functools

import jax
import jax.numpy as jnp
from jax import lax
from jax.experimental import pallas as pl
from jax.experimental.pallas import tpu as pltpu
from jax.sharding import PartitionSpec as P

F32 = jnp.float32
BF16 = jnp.bfloat16
MESH = pl.DeviceIdType.MESH
PIECES = 8
SHARE = 2
HIGHEST = lax.Precision.HIGHEST


def flip(index, bit):
    return index + bit * (1 - 2 * ((index // bit) % 2))


def split_dot(left, right):
    if right.dtype == BF16:
        return jnp.dot(left, right, preferred_element_type=F32)
    high = right.astype(BF16)
    low = (right - high.astype(F32)).astype(BF16)
    return jnp.dot(left, high, preferred_element_type=F32) + jnp.dot(
        left, low, preferred_element_type=F32
    )


def kernel(
    n_sp, n_dp, heads, gather,
    q_hbm, k_hbm, v_hbm, gate_hbm, in_hbm, forget_hbm, w_ref, o_ref,
    q_ref, k_ref, v_ref, gate_ref, in_ref, forget_ref, load_sem,
    q_next, prod_in, prod_out, q_sem,
    rows_ref, cols_ref, kw_ref, nloc_ref, kv_ref, num_ref, gated_ref,
    aux_in, aux_out, state_in, state_out, aux_sem, state_send, state_recv,
    *w_scratch,
):
    z = lax.axis_index("sp")
    d = lax.axis_index("dp")
    tokens = q_ref.shape[1]
    dk = q_ref.shape[2] // heads
    dv = v_ref.shape[2] // heads
    scale = dk ** (-0.5)
    total = state_in.shape[0]
    per_head = total // heads
    wide = state_in.shape[2]
    last = n_sp - 1
    relay = n_sp > 2 and tokens < dk

    def q_copy(target):
        return pltpu.make_async_remote_copy(
            src_ref=q_ref.at[0], dst_ref=q_next, send_sem=q_sem.at[0], recv_sem=q_sem.at[1],
            device_id={"sp": target}, device_id_type=MESH,
        )


    barrier = pltpu.get_barrier_semaphore()
    loads = [
        pltpu.make_async_copy(source, target, load_sem.at[n])
        for n, (source, target) in enumerate(
            (
                (in_hbm, in_ref),
                (forget_hbm, forget_ref),
                (k_hbm, k_ref),
                (v_hbm, v_ref),
                (q_hbm, q_ref),
                (gate_hbm, gate_ref),
            )
        )
    ]
    for load in loads:
        load.start()
    count = 0
    if gather:
        for bit in (1, 2, 4):
            pl.semaphore_signal(barrier, 1, device_id={"dp": flip(d, bit)}, device_id_type=MESH)
        count = 3

    @pl.when(z > 0)
    def _():
        pl.semaphore_signal(barrier, 1, device_id={"sp": z - 1}, device_id_type=MESH)

    @pl.when(z < last)
    def _():
        pl.semaphore_signal(barrier, 1, device_id={"sp": z + 1}, device_id_type=MESH)

    count = count + jnp.where(z > 0, 1, 0) + jnp.where(z < last, 1, 0)
    pl.semaphore_wait(barrier, count)

    if gather:
        w_all, own_sem, w_send, w_recv = w_scratch
        core, xp, yp = flip(d, 1), flip(d, 2), flip(d, 4)
        diag = flip(xp, 4)
        core_x, core_y, core_diag = flip(xp, 1), flip(yp, 1), flip(diag, 1)
        deep = w_ref.shape[0] // PIECES
        half = PIECES // 2
        odd = z % 2
        fresh = [n + SHARE * odd for n in range(SHARE)]
        shared = [n + SHARE * (1 - odd) for n in range(SHARE)]
        rest = list(range(2 * SHARE, PIECES))
        cut = half - SHARE
        x_order = fresh + rest[:cut] + rest[cut:]
        y_order = shared + rest[cut : 2 * cut] + rest[:cut] + rest[2 * cut :]
        to_y, to_x = x_order[:half], y_order[:half]
        direct = PIECES - SHARE

        def part(piece):
            return pl.ds(pl.multiple_of(piece * deep, deep), deep)

        def copy_of(lane, piece, block, target, source=None, axis="dp"):
            rows = part(piece)
            src = w_all.at[block, rows] if source is None else source.at[rows]
            return pltpu.make_async_remote_copy(
                src_ref=src,
                dst_ref=w_all.at[block, rows],
                send_sem=w_send.at[lane, piece],
                recv_sem=w_recv.at[lane, piece],
                device_id={axis: target},
                device_id_type=MESH,
            )

        for x_piece, y_piece in zip(x_order[:direct], y_order[:direct]):
            copy_of(0, x_piece, d, xp, w_ref).start()
            copy_of(1, y_piece, d, yp, w_ref).start()
        for piece in range(PIECES):
            copy_of(3, piece, d, core, w_ref).start()
        own = pltpu.make_async_copy(w_ref, w_all.at[d], own_sem)
        own.start()

        def pass_on(step):
            for lane, order, block, target in ((0, x_order, xp, yp), (1, y_order, yp, xp)):
                piece = order[step]
                copy_of(lane, piece, block, block).wait_recv()
                if step < SHARE:

                    @pl.when(z == last - 1)
                    def _():
                        copy_of(9 + lane, piece, block, last, axis="sp").start()

                    @pl.when(z > 0)
                    def _():
                        copy_of(7 + lane, piece, block, z - 1, axis="sp").start()

                if step < half:
                    copy_of(2, piece, block, target).start()
                copy_of(4 + lane, piece, block, core).start()

    for load in loads:
        load.wait()
    if relay:

        @pl.when(z == last)
        def _():
            q_copy(last - 1).start()

    forget = forget_ref[0].astype(F32)
    gain = in_ref[0].astype(F32)
    decay = -(jnp.log1p(jnp.exp(-jnp.abs(forget))) + jnp.maximum(-forget, 0.0))
    row_id = lax.broadcasted_iota(jnp.int32, (tokens, tokens), 0)
    col_id = lax.broadcasted_iota(jnp.int32, (tokens, tokens), 1)
    running = jnp.dot(
        decay, (row_id <= col_id).astype(F32), precision=HIGHEST, preferred_element_type=F32
    )
    offset = gain - running
    end = running[:, tokens - 1 : tokens]
    top_here = end + jnp.max(offset, axis=1, keepdims=True)
    weight = jnp.exp(end + offset - top_here)
    rows_ref[...] = jnp.zeros_like(rows_ref)
    rows_ref[0:heads] = running
    rows_ref[heads : 2 * heads] = weight * scale
    cols_ref[...] = rows_ref[...].T

    for h in range(heads):
        keys = k_ref[0, :, h * dk : (h + 1) * dk].astype(F32)
        weighted = keys * cols_ref[:, heads + h : heads + h + 1]
        kw_ref[:, h * dk : (h + 1) * dk] = weighted.astype(BF16)
        nloc_ref[h : h + 1] = jnp.sum(weighted, axis=0, keepdims=True)

    def own_state(h):
        kv_ref[h] = lax.dot_general(
            kw_ref[:, h * dk : (h + 1) * dk],
            v_ref[0, :, h * dv : (h + 1) * dv],
            (((0,), (0,)), ((), ())),
            preferred_element_type=F32,
        )

    def aux_copy():
        return pltpu.make_async_remote_copy(
            src_ref=aux_out, dst_ref=aux_in, send_sem=aux_sem.at[0], recv_sem=aux_sem.at[1],
            device_id={"sp": jnp.minimum(z + 1, last)}, device_id_type=MESH,
        )

    def state_copy(j):
        return pltpu.make_async_remote_copy(
            src_ref=state_out.at[j], dst_ref=state_in.at[j],
            send_sem=state_send.at[j], recv_sem=state_recv.at[j],
            device_id={"sp": jnp.minimum(z + 1, last)}, device_id_type=MESH,
        )

    def prod_copy(j):
        return pltpu.make_async_remote_copy(
            src_ref=prod_out.at[j], dst_ref=prod_in.at[j],
            send_sem=state_send.at[j], recv_sem=state_recv.at[j],
            device_id={"sp": jnp.minimum(z + 1, last)}, device_id_type=MESH,
        )

    def aux_step(m, normer):
        top = jnp.maximum(end + m, top_here)
        keep = jnp.exp(end + m - top)
        add = jnp.exp(top_here - top)
        aux_out[0:heads] = keep * normer + add * nloc_ref[...]
        aux_out[heads : 2 * heads] = jnp.broadcast_to(top, (heads, dk))
        return keep, add

    def chunk_of(j):
        h, c = j // per_head, j % per_head
        return h, slice(c * wide, (c + 1) * wide), slice(h * dv + c * wide, h * dv + (c + 1) * wide)

    @pl.when(z == 0)
    def _():
        zero = jnp.zeros((heads, 1), F32)
        _, add = aux_step(zero, jnp.zeros((heads, dk), F32))
        aux_copy().start()
        for h in range(heads):
            own_state(h)
            for c in range(per_head):
                j = h * per_head + c
                _, inner, _ = chunk_of(j)
                state_out[j] = (add[h : h + 1] * kv_ref[h, :, inner]).astype(state_out.dtype)
                state_copy(j).start()
        aux_in[...] = jnp.zeros_like(aux_in)
        state_in[...] = jnp.zeros_like(state_in)

    @pl.when((z > 0) & (z < last))
    def _():
        for h in range(heads):
            own_state(h)

    tops, dens = [], []
    for h in range(heads):
        query = q_ref[0, :, h * dk : (h + 1) * dk]
        raw = lax.dot_general(
            query, k_ref[0, :, h * dk : (h + 1) * dk], (((1,), (1,)), ((), ())),
            preferred_element_type=F32,
        )
        log_weight = cols_ref[:, h : h + 1] + offset[h : h + 1]
        log_weight = jnp.where(row_id >= col_id, log_weight, -jnp.inf)
        top = jnp.max(log_weight, axis=1, keepdims=True)
        scores = (raw * scale) * jnp.exp(log_weight - top)
        tops.append(top)
        dens.append(jnp.sum(scores, axis=1, keepdims=True))
        high = scores.astype(BF16)
        low = (scores - high.astype(F32)).astype(BF16)
        value = v_ref[0, :, h * dv : (h + 1) * dv]
        num_ref[:, h * dv : (h + 1) * dv] = jnp.dot(
            high, value, preferred_element_type=F32
        ) + jnp.dot(low, value, preferred_element_type=F32)

    @pl.when(z > 0)
    def _():
        aux_copy().wait_recv()

    m = aux_in[heads : 2 * heads, 0:1]

    @pl.when((z > 0) & (z < last))
    def _():
        aux_step(m, aux_in[0:heads])
        aux_copy().start()

    top_next = jnp.maximum(end + m, top_here)
    keep = jnp.exp(end + m - top_next)
    add = jnp.exp(top_here - top_next)

    for j in range(total):
        h, inner, outer = chunk_of(j)
        if gather:
            for step in range(half):
                place = [min(max(2 * step + 2 - (5 * s) // 2, 0), total - 1) for s in range(n_sp)]
                hits = [s for s in range(n_sp) if place[s] == j]
                if hits:

                    @pl.when((z >= hits[0]) & (z <= hits[-1]))
                    def _(step=step):
                        pass_on(step)

        def step_state():
            return keep[h : h + 1] * state_in[j].astype(F32) + add[h : h + 1] * kv_ref[h, :, inner]

        @pl.when((z > 0) & (z < (last if relay else n_sp)))
        def _():
            state_copy(j).wait_recv()

        @pl.when((z > 0) & (z < (last - 1 if relay else last)))
        def _():
            state_out[j] = step_state().astype(state_out.dtype)
            state_copy(j).start()

        if relay:

            @pl.when(z == last - 1)
            def _():
                if j == 0:
                    q_copy(last - 1).wait_recv()
                prod_out[j] = split_dot(
                    q_next[:, h * dk : (h + 1) * dk], step_state().astype(state_out.dtype)
                ).astype(prod_out.dtype)
                prod_copy(j).start()

        query = q_ref[0, :, h * dk : (h + 1) * dk]
        if j % per_head == 0:
            carried = cols_ref[:, h : h + 1] + m[h : h + 1]
            top = jnp.maximum(carried, tops[h])
            local = jnp.exp(tops[h] - top)
            past = jnp.exp(carried - top)
            den = local * dens[h] + past * jnp.sum(
                query.astype(F32) * aux_in[h : h + 1], axis=1, keepdims=True
            )
            inverse = 1.0 / jnp.maximum(jnp.abs(den), 1.0)
            local, past = local * inverse, past * inverse
        def finish(product):
            cell = local * num_ref[:, outer] + past * product
            hidden = cell.astype(BF16).astype(F32)
            gate = jax.nn.sigmoid(gate_ref[0, :, outer].astype(F32))
            gated_ref[:, outer] = (hidden * gate).astype(BF16)

        if relay:

            @pl.when(z < last)
            def _():
                finish(split_dot(query, state_in[j]))

            @pl.when(z == last)
            def _():
                prod_copy(j).wait_recv()
                finish(prod_in[j].astype(F32))

        else:
            finish(split_dot(query, state_in[j]))

    if not gather:
        o_ref[0] = jnp.dot(gated_ref[...], w_ref[...], preferred_element_type=F32).astype(BF16)
    else:
        cols = w_ref.shape[1]

        def column(block):
            return pl.ds(pl.multiple_of(block * cols, cols), cols)

        def project(block):
            o_ref[0, :, column(block)] = jnp.dot(
                gated_ref[...], w_all[block], preferred_element_type=F32
            ).astype(BF16)

        for step in range(half, direct):
            pass_on(step)
        own.wait()
        project(d)
        for n in range(SHARE):
            for lane, piece, block in ((0, shared[n], xp), (1, fresh[n], yp)):

                @pl.when(z < last)
                def _():
                    copy_of(7 + lane, piece, block, 0, axis="sp").wait_recv()

                @pl.when(z == last)
                def _():
                    copy_of(9 + lane, piece, block, 0, axis="sp").wait_recv()

                copy_of(4 + lane, piece, block, core).start()
        for piece in range(PIECES):
            copy_of(3, piece, core, core).wait_recv()
        project(core)
        project(xp)
        project(yp)
        for piece in range(PIECES):
            copy_of(4, piece, core_x, core).wait_recv()
        project(core_x)
        for piece in range(PIECES):
            copy_of(5, piece, core_y, core).wait_recv()
        project(core_y)
        mine = jnp.zeros((tokens, cols), F32)
        other = jnp.zeros((tokens, cols), F32)
        order = [p for pair in zip(to_y, to_x) for p in pair]
        for piece in order:
            copy_of(2, piece, diag, yp).wait_recv()
            copy_of(6, piece, diag, core).start()
            rows = part(piece)
            mine += jnp.dot(gated_ref[:, rows], w_all[diag, rows], preferred_element_type=F32)
        o_ref[0, :, column(diag)] = mine.astype(BF16)
        for piece in order:
            copy_of(6, piece, core_diag, core).wait_recv()
            rows = part(piece)
            other += jnp.dot(gated_ref[:, rows], w_all[core_diag, rows], preferred_element_type=F32)
        o_ref[0, :, column(core_diag)] = other.astype(BF16)
        for piece in range(PIECES):
            copy_of(3, piece, d, core, w_ref).wait_send()
            copy_of(4, piece, xp, core).wait_send()
            copy_of(5, piece, yp, core).wait_send()
            copy_of(6, piece, diag, core).wait_send()
        for step in range(direct):
            copy_of(0, x_order[step], d, xp, w_ref).wait_send()
            copy_of(1, y_order[step], d, yp, w_ref).wait_send()
        for step in range(half):
            copy_of(2, to_y[step], xp, yp).wait_send()
            copy_of(2, to_x[step], yp, xp).wait_send()
        for n in range(SHARE):
            for lane, piece, block in ((0, fresh[n], xp), (1, shared[n], yp)):

                @pl.when(z == last - 1)
                def _():
                    copy_of(9 + lane, piece, block, 0, axis="sp").wait_send()

                @pl.when(z > 0)
                def _():
                    copy_of(7 + lane, piece, block, 0, axis="sp").wait_send()

    if relay:

        @pl.when(z == last)
        def _():
            q_copy(last - 1).wait_send()

        @pl.when(z == last - 1)
        def _():
            aux_copy().wait_send()
            for j in range(total):
                prod_copy(j).wait_send()

    @pl.when(z < (last - 1 if relay else last))
    def _():
        aux_copy().wait_send()
        for j in range(total):
            state_copy(j).wait_send()


def body(n_sp, n_dp, queries, key_rows, values, out_gate, input_gate, forget_gate, out_weight):
    heads = input_gate.shape[1]
    tokens = queries.shape[1]
    dk = queries.shape[2] // heads
    width = values.shape[2]
    dv = width // heads
    wide = min(128, dv)
    total = heads * (dv // wide)
    state_type = BF16 if n_sp <= 4 else F32
    depth, cols = out_weight.shape
    gather = n_dp == 8 and cols % 128 == 0
    loaded = (queries, key_rows, values, out_gate, input_gate, forget_gate)
    scratch = [pltpu.VMEM(source.shape, source.dtype) for source in loaded] + [
        pltpu.SemaphoreType.DMA((len(loaded),)),
        pltpu.VMEM((tokens, heads * dk), BF16),
        pltpu.VMEM((total, tokens, wide), state_type),
        pltpu.VMEM((total, tokens, wide), state_type),
        pltpu.SemaphoreType.DMA((2,)),
        pltpu.VMEM((tokens, tokens), F32),
        pltpu.VMEM((tokens, tokens), F32),
        pltpu.VMEM((tokens, heads * dk), BF16),
        pltpu.VMEM((heads, dk), F32),
        pltpu.VMEM((heads, dk, dv), F32),
        pltpu.VMEM((tokens, width), F32),
        pltpu.VMEM((tokens, width), BF16),
        pltpu.VMEM((2 * heads, dk), F32),
        pltpu.VMEM((2 * heads, dk), F32),
        pltpu.VMEM((total, dk, wide), state_type),
        pltpu.VMEM((total, dk, wide), state_type),
        pltpu.SemaphoreType.DMA((2,)),
        pltpu.SemaphoreType.DMA((total,)),
        pltpu.SemaphoreType.DMA((total,)),
    ]
    vmem = pl.BlockSpec(memory_space=pltpu.VMEM)
    w_spec = vmem
    if gather:
        scratch += [
            pltpu.VMEM((n_dp, depth, cols), BF16),
            pltpu.SemaphoreType.DMA,
            pltpu.SemaphoreType.DMA((11, PIECES)),
            pltpu.SemaphoreType.DMA((11, PIECES)),
        ]
        w_spec = pl.BlockSpec(memory_space=pl.ANY)
    else:
        out_weight = lax.all_gather(out_weight, "dp", axis=1, tiled=True)
    out_width = cols * n_dp
    return pl.pallas_call(
        functools.partial(kernel, n_sp, n_dp, heads, gather),
        out_shape=jax.ShapeDtypeStruct((1, tokens, out_width), BF16),
        in_specs=[pl.BlockSpec(memory_space=pl.ANY)] * 6 + [w_spec],
        out_specs=vmem,
        scratch_shapes=scratch,
        compiler_params=pltpu.CompilerParams(
            collective_id=0, has_side_effects=True, vmem_limit_bytes=56 * 1024 * 1024
        ),
    )(queries, key_rows, values, out_gate, input_gate, forget_gate, out_weight)


def solution(mesh):
    n_sp, n_dp = mesh.shape["sp"], mesh.shape["dp"]
    return jax.shard_map(
        functools.partial(body, n_sp, n_dp),
        mesh=mesh,
        in_specs=(
            P("dp", "sp", None),
            P("dp", "sp", None),
            P("dp", "sp", None),
            P("dp", "sp", None),
            P("dp", None, "sp"),
            P("dp", None, "sp"),
            P(None, "dp"),
        ),
        out_specs=P("dp", "sp", None),
        check_vma=False,
    )
```

```python
import functools

import jax
import jax.numpy as jnp
from jax import lax
from jax.experimental import pallas as pl
from jax.experimental.pallas import tpu as pltpu
from jax.sharding import PartitionSpec as P

F32 = jnp.float32
BF16 = jnp.bfloat16
MESH = pl.DeviceIdType.MESH
PIECES = 8
SHARE = 2
VMEM_BYTES = 67_043_328
HIGHEST = lax.Precision.HIGHEST


def flip(index, bit):
    return index + bit * (1 - 2 * ((index // bit) % 2))


def split_dot(left, right):
    if right.dtype == BF16:
        return jnp.dot(left, right, preferred_element_type=F32)
    high = right.astype(BF16)
    low = (right - high.astype(F32)).astype(BF16)
    return jnp.dot(left, high, preferred_element_type=F32) + jnp.dot(
        left, low, preferred_element_type=F32
    )


def kernel(
    n_sp, n_dp, heads, gather,
    q_hbm, k_hbm, v_hbm, gate_hbm, in_hbm, forget_hbm, w_ref, o_ref,
    q_ref, k_ref, v_ref, gate_ref, in_ref, forget_ref, load_sem,
    q_next, prod_in, prod_out, q_sem,
    rows_ref, cols_ref, kw_ref, nloc_ref, kv_ref, num_ref, gated_ref,
    aux_in, aux_out, state_in, state_out, aux_sem, state_send, state_recv,
    *w_scratch,
):
    z = lax.axis_index("sp")
    d = lax.axis_index("dp")
    tokens = q_ref.shape[1]
    dk = q_ref.shape[2] // heads
    dv = v_ref.shape[2] // heads
    scale = dk ** (-0.5)
    total = state_in.shape[0]
    per_head = total // heads
    wide = state_in.shape[2]
    last = n_sp - 1
    relay = n_sp > 2 and tokens < dk

    def q_copy(target):
        return pltpu.make_async_remote_copy(
            src_ref=q_ref.at[0], dst_ref=q_next, send_sem=q_sem.at[0], recv_sem=q_sem.at[1],
            device_id={"sp": target}, device_id_type=MESH,
        )


    barrier = pltpu.get_barrier_semaphore()
    loads = [
        pltpu.make_async_copy(source, target, load_sem.at[n])
        for n, (source, target) in enumerate(
            (
                (in_hbm, in_ref),
                (forget_hbm, forget_ref),
                (k_hbm, k_ref),
                (v_hbm, v_ref),
                (q_hbm, q_ref),
                (gate_hbm, gate_ref),
            )
        )
    ]
    for load in loads:
        load.start()
    count = 0
    if gather:
        for bit in (1, 2, 4):
            pl.semaphore_signal(barrier, 1, device_id={"dp": flip(d, bit)}, device_id_type=MESH)
        count = 3

    @pl.when(z > 0)
    def _():
        pl.semaphore_signal(barrier, 1, device_id={"sp": z - 1}, device_id_type=MESH)

    @pl.when(z < last)
    def _():
        pl.semaphore_signal(barrier, 1, device_id={"sp": z + 1}, device_id_type=MESH)

    count = count + jnp.where(z > 0, 1, 0) + jnp.where(z < last, 1, 0)
    pl.semaphore_wait(barrier, count)

    if gather:
        w_all, acc_ref, own_sem, w_send, w_recv = w_scratch
        core, xp, yp = flip(d, 1), flip(d, 2), flip(d, 4)
        diag = flip(xp, 4)
        core_x, core_y, core_diag = flip(xp, 1), flip(yp, 1), flip(diag, 1)
        deep = w_ref.shape[0] // PIECES
        half = PIECES // 2
        odd = z % 2
        fresh = [n + SHARE * odd for n in range(SHARE)]
        shared = [n + SHARE * (1 - odd) for n in range(SHARE)]
        rest = list(range(2 * SHARE, PIECES))
        cut = half - SHARE
        x_order = fresh + rest[:cut] + rest[cut:]
        y_order = shared + rest[cut : 2 * cut] + rest[:cut] + rest[2 * cut :]
        to_y, to_x = x_order[:half], y_order[:half]
        direct = PIECES - SHARE

        def part(piece):
            return pl.ds(pl.multiple_of(piece * deep, deep), deep)

        def copy_of(lane, piece, block, target, source=None, axis="dp"):
            rows = part(piece)
            src = w_all.at[block, rows] if source is None else source.at[rows]
            return pltpu.make_async_remote_copy(
                src_ref=src,
                dst_ref=w_all.at[block, rows],
                send_sem=w_send.at[lane, piece],
                recv_sem=w_recv.at[lane, piece],
                device_id={axis: target},
                device_id_type=MESH,
            )

        for x_piece, y_piece in zip(x_order[:direct], y_order[:direct]):
            copy_of(0, x_piece, d, xp, w_ref).start()
            copy_of(1, y_piece, d, yp, w_ref).start()
        for piece in range(PIECES):
            copy_of(3, piece, d, core, w_ref).start()
        own = pltpu.make_async_copy(w_ref, w_all.at[d], own_sem)
        own.start()

        def pass_on(step):
            for lane, order, block, target in ((0, x_order, xp, yp), (1, y_order, yp, xp)):
                piece = order[step]
                copy_of(lane, piece, block, block).wait_recv()
                if step < SHARE:

                    @pl.when(z == last - 1)
                    def _():
                        copy_of(9 + lane, piece, block, last, axis="sp").start()

                    @pl.when(z > 0)
                    def _():
                        copy_of(7 + lane, piece, block, z - 1, axis="sp").start()

                if step < half:
                    copy_of(2, piece, block, target).start()
                copy_of(4 + lane, piece, block, core).start()

    for load in loads:
        load.wait()
    if relay:

        @pl.when(z == last)
        def _():
            q_copy(last - 1).start()

    forget = forget_ref[0].astype(F32)
    gain = in_ref[0].astype(F32)
    decay = -(jnp.log1p(jnp.exp(-jnp.abs(forget))) + jnp.maximum(-forget, 0.0))
    row_id = lax.broadcasted_iota(jnp.int32, (tokens, tokens), 0)
    col_id = lax.broadcasted_iota(jnp.int32, (tokens, tokens), 1)
    running = jnp.dot(
        decay, (row_id <= col_id).astype(F32), precision=HIGHEST, preferred_element_type=F32
    )
    offset = gain - running
    end = running[:, tokens - 1 : tokens]
    top_here = end + jnp.max(offset, axis=1, keepdims=True)
    weight = jnp.exp(end + offset - top_here)
    rows_ref[...] = jnp.zeros_like(rows_ref)
    rows_ref[0:heads] = running
    rows_ref[heads : 2 * heads] = weight * scale
    cols_ref[...] = rows_ref[...].T

    for h in range(heads):
        keys = k_ref[0, :, h * dk : (h + 1) * dk].astype(F32)
        weighted = keys * cols_ref[:, heads + h : heads + h + 1]
        kw_ref[:, h * dk : (h + 1) * dk] = weighted.astype(BF16)
        nloc_ref[h : h + 1] = jnp.sum(weighted, axis=0, keepdims=True)

    def own_state(h):
        kv_ref[h] = lax.dot_general(
            kw_ref[:, h * dk : (h + 1) * dk],
            v_ref[0, :, h * dv : (h + 1) * dv],
            (((0,), (0,)), ((), ())),
            preferred_element_type=F32,
        )

    def aux_copy():
        return pltpu.make_async_remote_copy(
            src_ref=aux_out, dst_ref=aux_in, send_sem=aux_sem.at[0], recv_sem=aux_sem.at[1],
            device_id={"sp": jnp.minimum(z + 1, last)}, device_id_type=MESH,
        )

    def state_copy(j):
        return pltpu.make_async_remote_copy(
            src_ref=state_out.at[j], dst_ref=state_in.at[j],
            send_sem=state_send.at[j], recv_sem=state_recv.at[j],
            device_id={"sp": jnp.minimum(z + 1, last)}, device_id_type=MESH,
        )

    def prod_copy(j):
        return pltpu.make_async_remote_copy(
            src_ref=prod_out.at[j], dst_ref=prod_in.at[j],
            send_sem=state_send.at[j], recv_sem=state_recv.at[j],
            device_id={"sp": jnp.minimum(z + 1, last)}, device_id_type=MESH,
        )

    def aux_step(m, normer):
        top = jnp.maximum(end + m, top_here)
        keep = jnp.exp(end + m - top)
        add = jnp.exp(top_here - top)
        aux_out[0:heads] = keep * normer + add * nloc_ref[...]
        aux_out[heads : 2 * heads] = jnp.broadcast_to(top, (heads, dk))
        return keep, add

    def chunk_of(j):
        h, c = j // per_head, j % per_head
        return h, slice(c * wide, (c + 1) * wide), slice(h * dv + c * wide, h * dv + (c + 1) * wide)

    @pl.when(z == 0)
    def _():
        zero = jnp.zeros((heads, 1), F32)
        _, add = aux_step(zero, jnp.zeros((heads, dk), F32))
        aux_copy().start()
        for h in range(heads):
            own_state(h)
            for c in range(per_head):
                j = h * per_head + c
                _, inner, _ = chunk_of(j)
                state_out[j] = (add[h : h + 1] * kv_ref[h, :, inner]).astype(state_out.dtype)
                state_copy(j).start()
        aux_in[...] = jnp.zeros_like(aux_in)
        state_in[...] = jnp.zeros_like(state_in)

    @pl.when((z > 0) & (z < last))
    def _():
        own_state(0)

    def own_rows(h):
        query = q_ref[0, :, h * dk : (h + 1) * dk]
        raw = lax.dot_general(
            query, k_ref[0, :, h * dk : (h + 1) * dk], (((1,), (1,)), ((), ())),
            preferred_element_type=F32,
        )
        log_weight = cols_ref[:, h : h + 1] + offset[h : h + 1]
        log_weight = jnp.where(row_id >= col_id, log_weight, -jnp.inf)
        top = jnp.max(log_weight, axis=1, keepdims=True)
        scores = (raw * scale) * jnp.exp(log_weight - top)
        high = scores.astype(BF16)
        low = (scores - high.astype(F32)).astype(BF16)
        value = v_ref[0, :, h * dv : (h + 1) * dv]
        num_ref[:, h * dv : (h + 1) * dv] = jnp.dot(
            high, value, preferred_element_type=F32
        ) + jnp.dot(low, value, preferred_element_type=F32)
        return top, jnp.sum(scores, axis=1, keepdims=True)

    @pl.when(z > 0)
    def _():
        aux_copy().wait_recv()

    m = aux_in[heads : 2 * heads, 0:1]

    @pl.when((z > 0) & (z < last))
    def _():
        aux_step(m, aux_in[0:heads])
        aux_copy().start()

    top_next = jnp.maximum(end + m, top_here)
    keep = jnp.exp(end + m - top_next)
    add = jnp.exp(top_here - top_next)

    if gather:
        cols = w_ref.shape[1]
        width = gated_ref.shape[1]
        early = slice(0, width - dv)
        late = slice(width - dv, width)
        pairs = list(zip(to_y, to_x))

        def column(block):
            return pl.ds(pl.multiple_of(block * cols, cols), cols)

        def begin(block):
            acc_ref[:, column(block)] = jnp.dot(
                gated_ref[:, early], w_all[block, early], preferred_element_type=F32
            )

        def end_of(block):
            o_ref[0, :, column(block)] = (
                acc_ref[:, column(block)]
                + jnp.dot(gated_ref[:, late], w_all[block, late], preferred_element_type=F32)
            ).astype(BF16)

        def rest_of_blocks():
            for step in range(half, direct):
                pass_on(step)
            for n in range(SHARE):
                for lane, piece, block in ((0, shared[n], xp), (1, fresh[n], yp)):

                    @pl.when(z < last)
                    def _():
                        copy_of(7 + lane, piece, block, 0, axis="sp").wait_recv()

                    @pl.when(z == last)
                    def _():
                        copy_of(9 + lane, piece, block, 0, axis="sp").wait_recv()

                    copy_of(4 + lane, piece, block, core).start()

        def diagonal(pair):
            for piece in pair:
                copy_of(2, piece, diag, yp).wait_recv()
                copy_of(6, piece, diag, core).start()

    for j in range(total):
        h, inner, outer = chunk_of(j)
        if gather and j == total - per_head - 2:
            rest_of_blocks()
        if gather:
            for step in range(half):
                place = [min(max(2 * step + 2 - (5 * s) // 2, 0), total - 1) for s in range(n_sp)]
                hits = [s for s in range(n_sp) if place[s] == j]
                if hits:

                    @pl.when((z >= hits[0]) & (z <= hits[-1]))
                    def _(step=step):
                        pass_on(step)

        def step_state():
            return keep[h : h + 1] * state_in[j].astype(F32) + add[h : h + 1] * kv_ref[h, :, inner]

        @pl.when((z > 0) & (z < (last if relay else n_sp)))
        def _():
            state_copy(j).wait_recv()

        @pl.when((z > 0) & (z < (last - 1 if relay else last)))
        def _():
            state_out[j] = step_state().astype(state_out.dtype)
            state_copy(j).start()

        if relay:

            @pl.when(z == last - 1)
            def _():
                if j == 0:
                    q_copy(last - 1).wait_recv()
                prod_out[j] = split_dot(
                    q_next[:, h * dk : (h + 1) * dk], step_state().astype(state_out.dtype)
                ).astype(prod_out.dtype)
                prod_copy(j).start()

        if j % per_head == per_head - 1 and h + 1 < heads:

            @pl.when((z > 0) & (z < last))
            def _():
                own_state(h + 1)

        query = q_ref[0, :, h * dk : (h + 1) * dk]
        if j % per_head == 0:
            top_own, den_own = own_rows(h)
            carried = cols_ref[:, h : h + 1] + m[h : h + 1]
            top = jnp.maximum(carried, top_own)
            local = jnp.exp(top_own - top)
            past = jnp.exp(carried - top)
            den = local * den_own + past * jnp.sum(
                query.astype(F32) * aux_in[h : h + 1], axis=1, keepdims=True
            )
            inverse = 1.0 / jnp.maximum(jnp.abs(den), 1.0)
            local, past = local * inverse, past * inverse
        def finish(product):
            cell = local * num_ref[:, outer] + past * product
            hidden = cell.astype(BF16).astype(F32)
            gate = jax.nn.sigmoid(gate_ref[0, :, outer].astype(F32))
            gated_ref[:, outer] = (hidden * gate).astype(BF16)

        if relay:

            @pl.when(z < last)
            def _():
                finish(split_dot(query, state_in[j]))

            @pl.when(z == last)
            def _():
                prod_copy(j).wait_recv()
                finish(prod_in[j].astype(F32))

        else:
            finish(split_dot(query, state_in[j]))

        if gather:
            ready = j - (total - per_head - 1)
            if ready == 0:
                own.wait()
                for piece in range(PIECES):
                    copy_of(3, piece, core, core).wait_recv()
                begin(d)
                begin(core)
            elif ready == 1:
                begin(xp)
                begin(yp)
            elif ready == 2:
                for piece in range(PIECES):
                    copy_of(4, piece, core_x, core).wait_recv()
                    copy_of(5, piece, core_y, core).wait_recv()
                begin(core_x)
                begin(core_y)
                diagonal(pairs[0])
            elif ready == 3:
                diagonal(pairs[1])

    if not gather:
        o_ref[0] = jnp.dot(gated_ref[...], w_ref[...], preferred_element_type=F32).astype(BF16)
    else:
        for block in (d, core, xp, yp, core_x, core_y):
            end_of(block)
        for pair in pairs[2:]:
            diagonal(pair)
        mine = jnp.dot(gated_ref[...], w_all[diag], preferred_element_type=F32)
        o_ref[0, :, column(diag)] = mine.astype(BF16)
        for piece in range(PIECES):
            copy_of(6, piece, core_diag, core).wait_recv()
        other = jnp.dot(gated_ref[...], w_all[core_diag], preferred_element_type=F32)
        o_ref[0, :, column(core_diag)] = other.astype(BF16)
        for piece in range(PIECES):
            copy_of(3, piece, d, core, w_ref).wait_send()
            copy_of(4, piece, xp, core).wait_send()
            copy_of(5, piece, yp, core).wait_send()
            copy_of(6, piece, diag, core).wait_send()
        for step in range(direct):
            copy_of(0, x_order[step], d, xp, w_ref).wait_send()
            copy_of(1, y_order[step], d, yp, w_ref).wait_send()
        for step in range(half):
            copy_of(2, to_y[step], xp, yp).wait_send()
            copy_of(2, to_x[step], yp, xp).wait_send()
        for n in range(SHARE):
            for lane, piece, block in ((0, fresh[n], xp), (1, shared[n], yp)):

                @pl.when(z == last - 1)
                def _():
                    copy_of(9 + lane, piece, block, 0, axis="sp").wait_send()

                @pl.when(z > 0)
                def _():
                    copy_of(7 + lane, piece, block, 0, axis="sp").wait_send()

    if relay:

        @pl.when(z == last)
        def _():
            q_copy(last - 1).wait_send()

        @pl.when(z == last - 1)
        def _():
            aux_copy().wait_send()
            for j in range(total):
                prod_copy(j).wait_send()

    @pl.when(z < (last - 1 if relay else last))
    def _():
        aux_copy().wait_send()
        for j in range(total):
            state_copy(j).wait_send()


def body(n_sp, n_dp, queries, key_rows, values, out_gate, input_gate, forget_gate, out_weight):
    heads = input_gate.shape[1]
    tokens = queries.shape[1]
    dk = queries.shape[2] // heads
    width = values.shape[2]
    dv = width // heads
    wide = min(128, dv)
    total = heads * (dv // wide)
    state_type = BF16 if n_sp <= 4 else F32
    depth, cols = out_weight.shape
    gather = n_dp == 8 and cols % 128 == 0
    loaded = (queries, key_rows, values, out_gate, input_gate, forget_gate)
    scratch = [pltpu.VMEM(source.shape, source.dtype) for source in loaded] + [
        pltpu.SemaphoreType.DMA((len(loaded),)),
        pltpu.VMEM((tokens, heads * dk), BF16),
        pltpu.VMEM((total, tokens, wide), state_type),
        pltpu.VMEM((total, tokens, wide), state_type),
        pltpu.SemaphoreType.DMA((2,)),
        pltpu.VMEM((tokens, tokens), F32),
        pltpu.VMEM((tokens, tokens), F32),
        pltpu.VMEM((tokens, heads * dk), BF16),
        pltpu.VMEM((heads, dk), F32),
        pltpu.VMEM((heads, dk, dv), F32),
        pltpu.VMEM((tokens, width), F32),
        pltpu.VMEM((tokens, width), BF16),
        pltpu.VMEM((2 * heads, dk), F32),
        pltpu.VMEM((2 * heads, dk), F32),
        pltpu.VMEM((total, dk, wide), state_type),
        pltpu.VMEM((total, dk, wide), state_type),
        pltpu.SemaphoreType.DMA((2,)),
        pltpu.SemaphoreType.DMA((total,)),
        pltpu.SemaphoreType.DMA((total,)),
    ]
    vmem = pl.BlockSpec(memory_space=pltpu.VMEM)
    w_spec = vmem
    if gather:
        scratch += [
            pltpu.VMEM((n_dp, depth, cols), BF16),
            pltpu.VMEM((tokens, cols * n_dp), F32),
            pltpu.SemaphoreType.DMA,
            pltpu.SemaphoreType.DMA((11, PIECES)),
            pltpu.SemaphoreType.DMA((11, PIECES)),
        ]
        w_spec = pl.BlockSpec(memory_space=pl.ANY)
    else:
        out_weight = lax.all_gather(out_weight, "dp", axis=1, tiled=True)
    out_width = cols * n_dp
    return pl.pallas_call(
        functools.partial(kernel, n_sp, n_dp, heads, gather),
        out_shape=pltpu.VMEM((1, tokens, out_width), BF16),
        in_specs=[pl.BlockSpec(memory_space=pl.ANY)] * 6 + [w_spec],
        out_specs=vmem,
        scratch_shapes=scratch,
        compiler_params=pltpu.CompilerParams(
            collective_id=0, has_side_effects=True, vmem_limit_bytes=VMEM_BYTES - 2 * tokens * out_width
        ),
    )(queries, key_rows, values, out_gate, input_gate, forget_gate, out_weight)


def solution(mesh):
    n_sp, n_dp = mesh.shape["sp"], mesh.shape["dp"]
    return jax.shard_map(
        functools.partial(body, n_sp, n_dp),
        mesh=mesh,
        in_specs=(
            P("dp", "sp", None),
            P("dp", "sp", None),
            P("dp", "sp", None),
            P("dp", "sp", None),
            P("dp", None, "sp"),
            P("dp", None, "sp"),
            P(None, "dp"),
        ),
        out_specs=P("dp", "sp", None),
        check_vma=False,
    )
```

```python
import functools

import jax
import jax.numpy as jnp
from jax import lax
from jax.experimental import pallas as pl
from jax.experimental.pallas import tpu as pltpu
from jax.sharding import PartitionSpec as P

F32 = jnp.float32
BF16 = jnp.bfloat16
MESH = pl.DeviceIdType.MESH
PIECES = 8
SHARE = 2
VMEM_BYTES = 67_043_328
HIGHEST = lax.Precision.HIGHEST


def flip(index, bit):
    return index + bit * (1 - 2 * ((index // bit) % 2))


def split_dot(left, right):
    if right.dtype == BF16:
        return jnp.dot(left, right, preferred_element_type=F32)
    high = right.astype(BF16)
    low = (right - high.astype(F32)).astype(BF16)
    return jnp.dot(left, high, preferred_element_type=F32) + jnp.dot(
        left, low, preferred_element_type=F32
    )


def kernel(
    n_sp, n_dp, heads, gather,
    q_hbm, k_hbm, v_hbm, gate_hbm, in_hbm, forget_hbm, w_ref, o_ref,
    q_ref, k_ref, v_ref, gate_ref, in_ref, forget_ref, load_sem,
    q_next, prod_in, prod_out, q_sem,
    rows_ref, cols_ref, kw_ref, nloc_ref, kv_ref, num_ref, gated_ref,
    aux_in, aux_out, state_in, state_out, aux_sem, state_send, state_recv,
    *w_scratch,
):
    z = lax.axis_index("sp")
    d = lax.axis_index("dp")
    tokens = q_ref.shape[1]
    dk = q_ref.shape[2] // heads
    dv = v_ref.shape[2] // heads
    scale = dk ** (-0.5)
    total = state_in.shape[0]
    per_head = total // heads
    wide = state_in.shape[2]
    last = n_sp - 1
    relay = n_sp > 2 and tokens < dk

    def q_copy(target):
        return pltpu.make_async_remote_copy(
            src_ref=q_ref.at[0], dst_ref=q_next, send_sem=q_sem.at[0], recv_sem=q_sem.at[1],
            device_id={"sp": target}, device_id_type=MESH,
        )


    barrier = pltpu.get_barrier_semaphore()
    loads = [
        pltpu.make_async_copy(source, target, load_sem.at[n])
        for n, (source, target) in enumerate(
            (
                (in_hbm, in_ref),
                (forget_hbm, forget_ref),
                (k_hbm, k_ref),
                (v_hbm, v_ref),
                (q_hbm, q_ref),
                (gate_hbm, gate_ref),
            )
        )
    ]
    for load in loads:
        load.start()
    count = 0
    if gather:
        for bit in (1, 2, 4):
            pl.semaphore_signal(barrier, 1, device_id={"dp": flip(d, bit)}, device_id_type=MESH)
        count = 3

    @pl.when(z > 0)
    def _():
        pl.semaphore_signal(barrier, 1, device_id={"sp": z - 1}, device_id_type=MESH)

    @pl.when(z < last)
    def _():
        pl.semaphore_signal(barrier, 1, device_id={"sp": z + 1}, device_id_type=MESH)

    count = count + jnp.where(z > 0, 1, 0) + jnp.where(z < last, 1, 0)
    pl.semaphore_wait(barrier, count)

    if gather:
        w_all, acc_ref, own_sem, w_send, w_recv = w_scratch
        core, xp, yp = flip(d, 1), flip(d, 2), flip(d, 4)
        diag = flip(xp, 4)
        core_x, core_y, core_diag = flip(xp, 1), flip(yp, 1), flip(diag, 1)
        deep = w_ref.shape[0] // PIECES
        half = PIECES // 2
        odd = z % 2
        fresh = [n + SHARE * odd for n in range(SHARE)]
        shared = [n + SHARE * (1 - odd) for n in range(SHARE)]
        rest = list(range(2 * SHARE, PIECES))
        cut = half - SHARE
        x_order = fresh + rest[:cut] + rest[cut:]
        y_order = shared + rest[cut : 2 * cut] + rest[:cut] + rest[2 * cut :]
        to_y, to_x = x_order[:half], y_order[:half]
        direct = PIECES - SHARE

        def part(piece):
            return pl.ds(pl.multiple_of(piece * deep, deep), deep)

        def copy_of(lane, piece, block, target, source=None, axis="dp"):
            rows = part(piece)
            src = w_all.at[block, rows] if source is None else source.at[rows]
            return pltpu.make_async_remote_copy(
                src_ref=src,
                dst_ref=w_all.at[block, rows],
                send_sem=w_send.at[lane, piece],
                recv_sem=w_recv.at[lane, piece],
                device_id={axis: target},
                device_id_type=MESH,
            )

        for x_piece, y_piece in zip(x_order[:direct], y_order[:direct]):
            copy_of(0, x_piece, d, xp, w_ref).start()
            copy_of(1, y_piece, d, yp, w_ref).start()
        for piece in range(PIECES):
            copy_of(3, piece, d, core, w_ref).start()
        own = pltpu.make_async_copy(w_ref, w_all.at[d], own_sem)
        own.start()

        def pass_on(step):
            for lane, order, block, target in ((0, x_order, xp, yp), (1, y_order, yp, xp)):
                piece = order[step]
                copy_of(lane, piece, block, block).wait_recv()
                if step < SHARE:

                    @pl.when(z == last - 1)
                    def _():
                        copy_of(9 + lane, piece, block, last, axis="sp").start()

                    @pl.when(z > 0)
                    def _():
                        copy_of(7 + lane, piece, block, z - 1, axis="sp").start()

                if step < half:
                    copy_of(2, piece, block, target).start()
                copy_of(4 + lane, piece, block, core).start()

    for load in loads:
        load.wait()
    if relay:

        @pl.when(z == last)
        def _():
            q_copy(last - 1).start()

    forget = forget_ref[0].astype(F32)
    gain = in_ref[0].astype(F32)
    decay = -(jnp.log1p(jnp.exp(-jnp.abs(forget))) + jnp.maximum(-forget, 0.0))
    row_id = lax.broadcasted_iota(jnp.int32, (tokens, tokens), 0)
    col_id = lax.broadcasted_iota(jnp.int32, (tokens, tokens), 1)
    running = jnp.dot(
        decay, (row_id <= col_id).astype(F32), precision=HIGHEST, preferred_element_type=F32
    )
    offset = gain - running
    end = running[:, tokens - 1 : tokens]
    top_here = end + jnp.max(offset, axis=1, keepdims=True)
    weight = jnp.exp(end + offset - top_here)
    rows_ref[...] = jnp.zeros_like(rows_ref)
    rows_ref[0:heads] = running
    rows_ref[heads : 2 * heads] = weight * scale
    cols_ref[...] = rows_ref[...].T

    for h in range(heads):
        keys = k_ref[0, :, h * dk : (h + 1) * dk].astype(F32)
        weighted = keys * cols_ref[:, heads + h : heads + h + 1]
        kw_ref[:, h * dk : (h + 1) * dk] = weighted.astype(BF16)
        nloc_ref[h : h + 1] = jnp.sum(weighted, axis=0, keepdims=True)

    def own_state(h):
        kv_ref[h] = lax.dot_general(
            kw_ref[:, h * dk : (h + 1) * dk],
            v_ref[0, :, h * dv : (h + 1) * dv],
            (((0,), (0,)), ((), ())),
            preferred_element_type=F32,
        )

    def aux_copy():
        return pltpu.make_async_remote_copy(
            src_ref=aux_out, dst_ref=aux_in, send_sem=aux_sem.at[0], recv_sem=aux_sem.at[1],
            device_id={"sp": jnp.minimum(z + 1, last)}, device_id_type=MESH,
        )

    def state_copy(j):
        return pltpu.make_async_remote_copy(
            src_ref=state_out.at[j], dst_ref=state_in.at[j],
            send_sem=state_send.at[j], recv_sem=state_recv.at[j],
            device_id={"sp": jnp.minimum(z + 1, last)}, device_id_type=MESH,
        )

    def prod_copy(j):
        return pltpu.make_async_remote_copy(
            src_ref=prod_out.at[j], dst_ref=prod_in.at[j],
            send_sem=state_send.at[j], recv_sem=state_recv.at[j],
            device_id={"sp": jnp.minimum(z + 1, last)}, device_id_type=MESH,
        )

    def aux_step(m, normer):
        top = jnp.maximum(end + m, top_here)
        keep = jnp.exp(end + m - top)
        add = jnp.exp(top_here - top)
        aux_out[0:heads] = keep * normer + add * nloc_ref[...]
        aux_out[heads : 2 * heads] = jnp.broadcast_to(top, (heads, dk))
        return keep, add

    def chunk_of(j):
        h, c = j // per_head, j % per_head
        return h, slice(c * wide, (c + 1) * wide), slice(h * dv + c * wide, h * dv + (c + 1) * wide)

    @pl.when(z == 0)
    def _():
        zero = jnp.zeros((heads, 1), F32)
        _, add = aux_step(zero, jnp.zeros((heads, dk), F32))
        aux_copy().start()
        for h in range(heads):
            own_state(h)
            for c in range(per_head):
                j = h * per_head + c
                _, inner, _ = chunk_of(j)
                state_out[j] = (add[h : h + 1] * kv_ref[h, :, inner]).astype(state_out.dtype)
                state_copy(j).start()
        aux_in[...] = jnp.zeros_like(aux_in)
        state_in[...] = jnp.zeros_like(state_in)

    @pl.when((z > 0) & (z < last))
    def _():
        own_state(0)

    def own_rows(h):
        query = q_ref[0, :, h * dk : (h + 1) * dk]
        raw = lax.dot_general(
            query, k_ref[0, :, h * dk : (h + 1) * dk], (((1,), (1,)), ((), ())),
            preferred_element_type=F32,
        )
        log_weight = cols_ref[:, h : h + 1] + offset[h : h + 1]
        log_weight = jnp.where(row_id >= col_id, log_weight, -jnp.inf)
        top = jnp.max(log_weight, axis=1, keepdims=True)
        scores = (raw * scale) * jnp.exp(log_weight - top)
        high = scores.astype(BF16)
        low = (scores - high.astype(F32)).astype(BF16)
        value = v_ref[0, :, h * dv : (h + 1) * dv]
        num_ref[:, h * dv : (h + 1) * dv] = jnp.dot(
            high, value, preferred_element_type=F32
        ) + jnp.dot(low, value, preferred_element_type=F32)
        return top, jnp.sum(scores, axis=1, keepdims=True)

    @pl.when(z > 0)
    def _():
        aux_copy().wait_recv()

    m = aux_in[heads : 2 * heads, 0:1]

    @pl.when((z > 0) & (z < last))
    def _():
        aux_step(m, aux_in[0:heads])
        aux_copy().start()

    top_next = jnp.maximum(end + m, top_here)
    keep = jnp.exp(end + m - top_next)
    add = jnp.exp(top_here - top_next)

    if gather:
        cols = w_ref.shape[1]
        width = gated_ref.shape[1]
        early = slice(0, width - dv)
        middle = slice(width - dv, width - wide)
        blocks = (d, core, xp, yp, core_x, core_y)
        pairs = list(zip(to_y, to_x))

        def column(block):
            return pl.ds(pl.multiple_of(block * cols, cols), cols)

        def begin(block):
            acc_ref[:, column(block)] = jnp.dot(
                gated_ref[:, early], w_all[block, early], preferred_element_type=F32
            )

        def more(block):
            acc_ref[:, column(block)] += jnp.dot(
                gated_ref[:, middle], w_all[block, middle], preferred_element_type=F32
            )

        def end_of(block, late):
            o_ref[0, :, column(block)] = (
                acc_ref[:, column(block)]
                + jnp.dot(gated_ref[:, late], w_all[block, late], preferred_element_type=F32)
            ).astype(BF16)

        def rest_of_blocks():
            for step in range(half, direct):
                pass_on(step)
            for n in range(SHARE):
                for lane, piece, block in ((0, shared[n], xp), (1, fresh[n], yp)):

                    @pl.when(z < last)
                    def _():
                        copy_of(7 + lane, piece, block, 0, axis="sp").wait_recv()

                    @pl.when(z == last)
                    def _():
                        copy_of(9 + lane, piece, block, 0, axis="sp").wait_recv()

                    copy_of(4 + lane, piece, block, core).start()

        def diagonal(pair):
            for piece in pair:
                copy_of(2, piece, diag, yp).wait_recv()
                copy_of(6, piece, diag, core).start()

    for j in range(total):
        h, inner, outer = chunk_of(j)
        if gather and j == total - per_head - 2:
            rest_of_blocks()
        if gather:
            for step in range(half):
                place = [min(max(2 * step + 4 - (5 * s) // 2, 0), total - 1) for s in range(n_sp)]
                hits = [s for s in range(n_sp) if place[s] == j]
                if hits:

                    @pl.when((z >= hits[0]) & (z <= hits[-1]))
                    def _(step=step):
                        pass_on(step)

        def step_state():
            return keep[h : h + 1] * state_in[j].astype(F32) + add[h : h + 1] * kv_ref[h, :, inner]

        @pl.when((z > 0) & (z < (last if relay else n_sp)))
        def _():
            state_copy(j).wait_recv()

        @pl.when((z > 0) & (z < (last - 1 if relay else last)))
        def _():
            state_out[j] = step_state().astype(state_out.dtype)
            state_copy(j).start()

        if relay:

            @pl.when(z == last - 1)
            def _():
                if j == 0:
                    q_copy(last - 1).wait_recv()
                prod_out[j] = split_dot(
                    q_next[:, h * dk : (h + 1) * dk], step_state().astype(state_out.dtype)
                ).astype(prod_out.dtype)
                prod_copy(j).start()

        if j % per_head == per_head - 1 and h + 1 < heads:

            @pl.when((z > 0) & (z < last))
            def _():
                own_state(h + 1)

        query = q_ref[0, :, h * dk : (h + 1) * dk]
        if j % per_head == 0:
            top_own, den_own = own_rows(h)
            carried = cols_ref[:, h : h + 1] + m[h : h + 1]
            top = jnp.maximum(carried, top_own)
            local = jnp.exp(top_own - top)
            past = jnp.exp(carried - top)
            den = local * den_own + past * jnp.sum(
                query.astype(F32) * aux_in[h : h + 1], axis=1, keepdims=True
            )
            inverse = 1.0 / jnp.maximum(jnp.abs(den), 1.0)
            local, past = local * inverse, past * inverse
        def finish(product):
            cell = local * num_ref[:, outer] + past * product
            hidden = cell.astype(BF16).astype(F32)
            gate = jax.nn.sigmoid(gate_ref[0, :, outer].astype(F32))
            gated_ref[:, outer] = (hidden * gate).astype(BF16)

        if relay:

            @pl.when(z < last)
            def _():
                finish(split_dot(query, state_in[j]))

            @pl.when(z == last)
            def _():
                prod_copy(j).wait_recv()
                finish(prod_in[j].astype(F32))

        else:
            finish(split_dot(query, state_in[j]))

        if gather:
            ready = j - (total - per_head - 1)
            if ready == 0:
                own.wait()
                for piece in range(PIECES):
                    copy_of(3, piece, core, core).wait_recv()
                begin(d)
                begin(core)
            elif ready == 1:
                begin(xp)
                begin(yp)
            elif ready == 2:
                for piece in range(PIECES):
                    copy_of(4, piece, core_x, core).wait_recv()
                    copy_of(5, piece, core_y, core).wait_recv()
                begin(core_x)
                begin(core_y)
                diagonal(pairs[0])
            elif ready == 3:
                diagonal(pairs[1])

                @pl.when(z == last)
                def _():
                    for block in blocks:
                        more(block)

    if not gather:
        o_ref[0] = jnp.dot(gated_ref[...], w_ref[...], preferred_element_type=F32).astype(BF16)
    else:
        @pl.when(z == last)
        def _():
            for block in blocks:
                end_of(block, slice(width - wide, width))

        @pl.when(z < last)
        def _():
            for block in blocks:
                end_of(block, slice(width - dv, width))

        for pair in pairs[2:]:
            diagonal(pair)
        mine = jnp.dot(gated_ref[...], w_all[diag], preferred_element_type=F32)
        o_ref[0, :, column(diag)] = mine.astype(BF16)
        for piece in range(PIECES):
            copy_of(6, piece, core_diag, core).wait_recv()
        other = jnp.dot(gated_ref[...], w_all[core_diag], preferred_element_type=F32)
        o_ref[0, :, column(core_diag)] = other.astype(BF16)
        for piece in range(PIECES):
            copy_of(3, piece, d, core, w_ref).wait_send()
            copy_of(4, piece, xp, core).wait_send()
            copy_of(5, piece, yp, core).wait_send()
            copy_of(6, piece, diag, core).wait_send()
        for step in range(direct):
            copy_of(0, x_order[step], d, xp, w_ref).wait_send()
            copy_of(1, y_order[step], d, yp, w_ref).wait_send()
        for step in range(half):
            copy_of(2, to_y[step], xp, yp).wait_send()
            copy_of(2, to_x[step], yp, xp).wait_send()
        for n in range(SHARE):
            for lane, piece, block in ((0, fresh[n], xp), (1, shared[n], yp)):

                @pl.when(z == last - 1)
                def _():
                    copy_of(9 + lane, piece, block, 0, axis="sp").wait_send()

                @pl.when(z > 0)
                def _():
                    copy_of(7 + lane, piece, block, 0, axis="sp").wait_send()

    if relay:

        @pl.when(z == last)
        def _():
            q_copy(last - 1).wait_send()

        @pl.when(z == last - 1)
        def _():
            aux_copy().wait_send()
            for j in range(total):
                prod_copy(j).wait_send()

    @pl.when(z < (last - 1 if relay else last))
    def _():
        aux_copy().wait_send()
        for j in range(total):
            state_copy(j).wait_send()


def body(n_sp, n_dp, queries, key_rows, values, out_gate, input_gate, forget_gate, out_weight):
    heads = input_gate.shape[1]
    tokens = queries.shape[1]
    dk = queries.shape[2] // heads
    width = values.shape[2]
    dv = width // heads
    wide = min(128, dv)
    total = heads * (dv // wide)
    state_type = BF16 if n_sp <= 4 else F32
    depth, cols = out_weight.shape
    gather = n_dp == 8 and cols % 128 == 0
    loaded = (queries, key_rows, values, out_gate, input_gate, forget_gate)
    scratch = [pltpu.VMEM(source.shape, source.dtype) for source in loaded] + [
        pltpu.SemaphoreType.DMA((len(loaded),)),
        pltpu.VMEM((tokens, heads * dk), BF16),
        pltpu.VMEM((total, tokens, wide), state_type),
        pltpu.VMEM((total, tokens, wide), state_type),
        pltpu.SemaphoreType.DMA((2,)),
        pltpu.VMEM((tokens, tokens), F32),
        pltpu.VMEM((tokens, tokens), F32),
        pltpu.VMEM((tokens, heads * dk), BF16),
        pltpu.VMEM((heads, dk), F32),
        pltpu.VMEM((heads, dk, dv), F32),
        pltpu.VMEM((tokens, width), F32),
        pltpu.VMEM((tokens, width), BF16),
        pltpu.VMEM((2 * heads, dk), F32),
        pltpu.VMEM((2 * heads, dk), F32),
        pltpu.VMEM((total, dk, wide), state_type),
        pltpu.VMEM((total, dk, wide), state_type),
        pltpu.SemaphoreType.DMA((2,)),
        pltpu.SemaphoreType.DMA((total,)),
        pltpu.SemaphoreType.DMA((total,)),
    ]
    vmem = pl.BlockSpec(memory_space=pltpu.VMEM)
    w_spec = vmem
    if gather:
        scratch += [
            pltpu.VMEM((n_dp, depth, cols), BF16),
            pltpu.VMEM((tokens, cols * n_dp), F32),
            pltpu.SemaphoreType.DMA,
            pltpu.SemaphoreType.DMA((11, PIECES)),
            pltpu.SemaphoreType.DMA((11, PIECES)),
        ]
        w_spec = pl.BlockSpec(memory_space=pl.ANY)
    else:
        out_weight = lax.all_gather(out_weight, "dp", axis=1, tiled=True)
    out_width = cols * n_dp
    return pl.pallas_call(
        functools.partial(kernel, n_sp, n_dp, heads, gather),
        out_shape=pltpu.VMEM((1, tokens, out_width), BF16),
        in_specs=[pl.BlockSpec(memory_space=pl.ANY)] * 6 + [w_spec],
        out_specs=vmem,
        scratch_shapes=scratch,
        compiler_params=pltpu.CompilerParams(
            collective_id=0, has_side_effects=True, vmem_limit_bytes=VMEM_BYTES - 2 * tokens * out_width
        ),
    )(queries, key_rows, values, out_gate, input_gate, forget_gate, out_weight)


def solution(mesh):
    n_sp, n_dp = mesh.shape["sp"], mesh.shape["dp"]
    return jax.shard_map(
        functools.partial(body, n_sp, n_dp),
        mesh=mesh,
        in_specs=(
            P("dp", "sp", None),
            P("dp", "sp", None),
            P("dp", "sp", None),
            P("dp", "sp", None),
            P("dp", None, "sp"),
            P("dp", None, "sp"),
            P(None, "dp"),
        ),
        out_specs=P("dp", "sp", None),
        check_vma=False,
    )
```
